256 devices in a mesh: grp: 4 (over y, x), ep: 32 (over z), tp: 2 (over core).
Axes of the slice: x: 2, y: 2, z: 32, core: 2. Of those that a mesh axis runs over, the one named last changes fastest.
The devices are a block of a 4x16x32 slice.
Arguments:
- tokens: bfloat16 [8192, 2048], P(('grp', 'ep')), parts along dimension 0, may hold values from -6 to 6
- routes: int32 [8192, 4], P(('grp', 'ep')), parts along dimension 0, may hold values from 0 to 31, all different within a row; in each aligned block of 64 rows (0 to 63, 64 to 127, ...) at most 16 rows name the same one
- gate_weights: float32 [8192, 4], P(('grp', 'ep')), parts along dimension 0, may hold values from 0.05 to 1
- w_gate: bfloat16 [32, 2048, 1280], P('ep', None, 'tp'), may hold values from -0.125 to 0.125
- w_up: bfloat16 [32, 2048, 1280], P('ep', None, 'tp'), may hold values from -0.125 to 0.125
- w_down: bfloat16 [32, 1280, 2048], P('ep', 'tp'), may hold values from -0.15625 to 0.15625
- norm_gain: float32 [2048], P('tp'), may hold values from 0.1 to 1.9
- norm_bias: float32 [2048], P('tp'), may hold values from -2 to 2
Outputs:
- normed: bfloat16 [8192, 2048], P(('grp', 'ep'), 'tp'), parts along dimension 0
The draws below stay inside these ranges and needn't reach their ends.
There are 4 independent parts, one for each index of `grp`. The reference program is written for one: setup_inputs(seed, part) draws one part's arguments, and reference() takes and returns one part's arrays. A program takes and returns all parts, laid end to end along the dimension named above; an argument that names none is the same for every part. Nothing has to cross between parts.
Inputs may be any that keep to these rules, and one draw needn't show every extreme that they name: `routes`: the rows of a token name distinct experts; in each aligned block of 64 rows (the tokens of one index of ep) no expert is named more than 16 times, a bound that some block reaches.
All inputs are finite; a program needn't handle non-finite values.
Results may differ from the reference program's by a relative error of at most 0.0037.
Values may be sent and summed in bfloat16 or wider, within the bound.
A program may use at most 64 MiB of HBM per device.

```python
import math
import jax
import jax.numpy as jnp
import numpy as np
from jax import lax

D = 2048
FF = 1280
TOP = 4
TOK_DEV = 64
EXPERTS = 32
CAP = 16
TOKENS = 2048
N_EP = 32
N_TP = 2


def block_scale(key, extent, split, low, high):
    def one(position, blocks):
        draws = jax.random.uniform(jax.random.fold_in(jax.random.fold_in(key, 6), position), (blocks,), jnp.float32, low / len(split), high / len(split))
        return jnp.repeat(jnp.exp(draws), extent[position] // blocks).reshape((-1,) + (1,) * (len(extent) - position - 1))

    level = one(*split[0])
    for cut in split[1:]:
        level = level * one(*cut)
    return level


def routed_block(key, own, number, rows, count, top, reach, lean):
    sequence = jax.random.permutation(key, count)
    crowded, usual = portions_of(count, rows * top, reach, lean, True), portions_of(count, rows * top, reach, lean, False)
    places = jnp.arange(count)

    def named(lengths, rotation):
        used = int((lengths > 0).sum())
        fixed = max(1, used // 4)
        shifted = fixed + (places - fixed + rotation * (used - fixed)) % max(1, count - fixed)
        return jnp.zeros((count,), jnp.int32).at[sequence[jnp.where(places < fixed, places, shifted)]].set(jnp.asarray(lengths, jnp.int32))

    lengths = jnp.where(number % 4 == 0, named(crowded, number // 4), named(usual, number - number // 4 - 1))
    mixed = jax.random.permutation(jax.random.fold_in(own, 3), count)
    donor, taker = mixed[0:count // 2 * 2:2], mixed[1:count // 2 * 2:2]
    room = jnp.minimum(lengths[donor] - 1, reach - lengths[taker]) // 2
    room = jnp.where((donor == sequence[0]) | (taker == sequence[0]) | (lengths[taker] == 0), 0, jnp.maximum(room, 0))
    shifted = jax.random.randint(jax.random.fold_in(own, 4), (count // 2,), 0, 1 << 20) % (room + 1)
    lengths = lengths.at[donor].add(-shifted).at[taker].add(shifted)
    items = jnp.searchsorted(jnp.cumsum(lengths), jnp.arange(rows * top), side="right").astype(jnp.int32)
    grid = items.reshape(top, rows).T
    grid = grid[jax.random.permutation(jax.random.fold_in(own, 1), rows)]
    rotation = jax.random.randint(jax.random.fold_in(own, 2), (rows, 1), 0, top)
    return jnp.take_along_axis(grid, (jnp.arange(top)[None, :] + rotation) % top, axis=1)


def portions_of(amount, total, limit, skew, full):
    portions = [(1 << 20) // math.isqrt(rank ** skew) + 1 for rank in range(1, amount + 1)]
    largest = limit if full else min(limit, max(-(-total // amount), total * portions[0] // sum(portions)))
    least = 1 if total - largest >= amount - 1 else 0
    given, rest = [largest] + [least] * (amount - 1), total - largest - least * (amount - 1)
    while rest > 0:
        movable = [i for i in range(1, amount) if given[i] < largest] or [i for i in range(1, amount) if given[i] < limit]
        whole, left = sum([portions[i] for i in movable]), rest
        for i in movable:
            addition = min(limit - given[i], max(1, left * portions[i] // whole), rest)
            given[i] = given[i] + addition
            rest = rest - addition
    return np.array(given)


def gaussian(rng, dims, deviation, bound, pieces=(), kind=jnp.bfloat16):
    values = deviation * jax.random.normal(rng, dims, jnp.float32)
    if pieces:
        values = values * block_scale(rng, dims, pieces, -0.22, 0.18)
    return jnp.clip(values, -bound, bound).astype(kind)


def setup_inputs(seed: int = 0, part: int = 0) -> dict:
    streams_of = jax.random.split(jax.random.key(seed), 9)
    own_keys = jax.random.split(jax.random.fold_in(streams_of[8], part), 9)
    tokens = gaussian(own_keys[0], (TOKENS, D), 1.0, 6.0, ((0, 32),))
    routes_keys = jax.random.split(jax.random.fold_in(own_keys[1], 1), TOKENS // TOK_DEV)
    routes_turns = jax.random.permutation(jax.random.fold_in(own_keys[1], 3), TOKENS // TOK_DEV)
    routes = jax.vmap(lambda own, number: routed_block(jax.random.fold_in(own_keys[1], 2), own, number, TOK_DEV, EXPERTS, TOP, CAP, 2))(routes_keys, routes_turns).reshape((TOKENS, TOP))
    gate_weights = jnp.clip(jnp.exp(math.log(1.0) - 2.9957323 * jax.random.uniform(own_keys[2], (TOKENS, TOP), jnp.float32) ** block_scale(own_keys[2], (TOKENS, TOP), ((0, 32),), -0.2, 0.2)), 0.05, 1.0)
    w_gate = gaussian(streams_of[3], (EXPERTS, D, FF), D ** -0.5, 0.125, ((0, 32), (2, 2)))
    w_up = gaussian(streams_of[4], (EXPERTS, D, FF), D ** -0.5, 0.125, ((0, 32), (2, 2)))
    w_down = gaussian(streams_of[5], (EXPERTS, FF, D), FF ** -0.5, 0.15625, ((0, 32), (1, 2)))
    norm_gain = jnp.clip(1.0 + 0.18 * jax.random.normal(streams_of[6], (D,), jnp.float32), 0.1, 1.9)
    norm_bias = gaussian(streams_of[7], (D,), 0.4, 2.0, ((0, 2),), jnp.float32)
    return {"tokens": tokens, "routes": routes, "gate_weights": gate_weights, "w_gate": w_gate, "w_up": w_up, "w_down": w_down, "norm_gain": norm_gain, "norm_bias": norm_bias}


residual_scale = 1.4142135
norm_eps = 1e-05

def reference(tokens, routes, gate_weights, w_gate, w_up, w_down, norm_gain, norm_bias):
    pair_list = routes.reshape(N_EP, TOK_DEV * TOP).astype(jnp.int32)
    onehot = (pair_list[..., None] == jnp.arange(EXPERTS, dtype=jnp.int32)).astype(jnp.int32)
    slots = lax.optimization_barrier(jnp.sum((jnp.cumsum(onehot, axis=1) - onehot) * onehot, axis=-1))
    blocks = tokens.reshape(N_EP, TOK_DEV, D).astype(jnp.float32)
    weights = gate_weights.reshape(N_EP, TOK_DEV, TOP).astype(jnp.float32)
    columns = jnp.arange(CAP, dtype=jnp.int32)
    half = FF // N_TP

    def one_expert(carry, inputs):
        expert, gate_w, up_w, down_w = inputs
        picked = ((pair_list == expert)[..., None] & (slots[..., None] == columns)).astype(jnp.float32)
        picked = picked.reshape(N_EP, TOK_DEV, TOP, CAP)
        placed = lax.optimization_barrier(jnp.sum(picked, axis=2))
        rows = jnp.einsum('stc,std->scd', placed, blocks, precision=lax.Precision.HIGHEST)
        rows = rows.astype(jnp.bfloat16).reshape(N_EP * CAP, D)
        gate = jnp.dot(rows, gate_w, preferred_element_type=jnp.float32)
        upper = jnp.dot(rows, up_w, preferred_element_type=jnp.float32)
        hidden = (jax.nn.silu(gate) * upper).astype(jnp.bfloat16)
        total = jnp.zeros((N_EP * CAP, D), jnp.float32)
        for index in range(N_TP):
            partial_sum = jnp.dot(hidden[:, index * half:(index + 1) * half], down_w[index * half:(index + 1) * half], preferred_element_type=jnp.float32)
            total = total + lax.optimization_barrier(partial_sum.astype(jnp.bfloat16)).astype(jnp.float32)
        output = lax.optimization_barrier(total.astype(jnp.bfloat16)).astype(jnp.float32)
        output = output.reshape(N_EP, CAP, D)
        mixing = jnp.einsum('stkc,stk->stc', picked, weights, precision=lax.Precision.HIGHEST)
        carry = carry + jnp.einsum('stc,scd->std', mixing, output, precision=lax.Precision.HIGHEST)
        return (carry, None)
    start = jnp.zeros((N_EP, TOK_DEV, D), jnp.float32)
    mixed, _ = lax.scan(one_expert, start, (jnp.arange(EXPERTS, dtype=jnp.int32), w_gate, w_up, w_down))
    mixture = lax.optimization_barrier(mixed.reshape(TOKENS, D).astype(jnp.bfloat16)).astype(jnp.float32)
    summed = residual_scale * tokens.astype(jnp.float32) + mixture
    mean = lax.optimization_barrier(jnp.mean(summed, axis=-1, keepdims=True))
    variance = lax.optimization_barrier(jnp.mean(jnp.square(summed - mean), axis=-1, keepdims=True))
    normed = (summed - mean) * lax.rsqrt(variance + norm_eps) * norm_gain + norm_bias
    return normed.astype(jnp.bfloat16)
```

```python
import jax
import jax.numpy as jnp
from jax import lax
from jax.sharding import PartitionSpec as P

residual_scale = 1.4142135
norm_eps = 1e-05


def shards(tokens, routes, gate_weights, w_gate, w_up, w_down, norm_gain, norm_bias):
    tp_index = lax.axis_index("tp")
    ep_index = lax.axis_index("ep")
    num_tp = lax.axis_size("tp")
    tok_rows, width = tokens.shape
    half_width = width // num_tp
    own_half = lax.dynamic_slice_in_dim(tokens, tp_index * half_width, half_width, 1)
    part = lax.all_gather(own_half, "ep", axis=0, tiled=True)
    everyone = lax.all_gather(part, "tp", axis=1, tiled=True)
    all_routes = lax.all_gather(routes, "ep", axis=0, tiled=True)
    all_gates = lax.all_gather(gate_weights, "ep", axis=0, tiled=True)
    weight = jnp.sum(jnp.where(all_routes == ep_index, all_gates, 0.0), axis=1)
    gate = jnp.dot(everyone, w_gate[0], preferred_element_type=jnp.float32)
    upper = jnp.dot(everyone, w_up[0], preferred_element_type=jnp.float32)
    hidden = (jax.nn.silu(gate) * upper).astype(jnp.bfloat16)
    partial_sum = jnp.dot(hidden, w_down[0], preferred_element_type=jnp.float32)
    weighted = (partial_sum * weight[:, None]).astype(jnp.bfloat16)
    mine = lax.psum_scatter(weighted, "tp", scatter_dimension=1, tiled=True)
    mixture = lax.psum_scatter(mine, "ep", scatter_dimension=0, tiled=True)
    summed = residual_scale * own_half.astype(jnp.float32) + mixture.astype(jnp.float32)
    row_sum, row_squares = lax.psum(
        (jnp.sum(summed, axis=1), jnp.sum(summed * summed, axis=1)), "tp"
    )
    mean = row_sum / width
    variance = row_squares / width - mean * mean
    normed = (summed - mean[:, None]) * lax.rsqrt(
        variance[:, None] + norm_eps
    ) * norm_gain + norm_bias
    return normed.astype(jnp.bfloat16)


def solution(mesh):
    in_specs = (
        P(("grp", "ep"), None),
        P(("grp", "ep"), None),
        P(("grp", "ep"), None),
        P("ep", None, "tp"),
        P("ep", None, "tp"),
        P("ep", "tp", None),
        P("tp"),
        P("tp"),
    )
    out_specs = P(("grp", "ep"), "tp")
    return jax.shard_map(shards, mesh=mesh, in_specs=in_specs, out_specs=out_specs, check_vma=False)
```

```python
import functools

import jax
import jax.numpy as jnp
from jax import lax
from jax.experimental import pallas as pl
from jax.experimental.pallas import tpu as pltpu
from jax.sharding import PartitionSpec as P

residual_scale = 1.4142135
norm_eps = 1e-05
col_groups = 4
ffn_rows = 128
ffn_cols = 256
bf16, f32 = jnp.bfloat16, jnp.float32


def moe_kernel(
    num_ep, num_experts,
    tokens, meta, w_gate, w_up, w_down, gain, bias, out,
    rows_in, metas, wg, wu, wd, gains, biases, weight_cols, hidden, sums, chain, own_out, other_out,
    disp_recv, disp_send, meta_recv, meta_send, comb_recv, comb_send, local_sems, pair_sems,
):
    me = lax.axis_index("ep")
    core = lax.axis_index("tp")
    other = 1 - core
    half = num_ep // 2
    own_tok = tokens.shape[0] // 2
    width = tokens.shape[1]
    cols = width // col_groups
    part = own_tok // 2
    ff_half = w_down.shape[1]
    ff = 2 * ff_half
    ff_tiles = ff // ffn_cols
    chunks = 2 * col_groups
    slot_rows = 2 * own_tok
    own_row = half * slot_rows - own_tok
    batches = half * slot_rows // ffn_rows
    pairs = half // 2
    first_pair = pairs // 2
    ahead = pairs - first_pair - 1
    last = batches - 1
    targets = ({"ep": lax.rem(me + 1, num_ep)}, {"ep": lax.rem(me + num_ep - 1, num_ep)})
    partner = {"tp": other}

    loads = []
    for g in range(col_groups):
        loads.append(pltpu.make_async_copy(
            tokens.at[pl.ds(core * own_tok, own_tok), pl.ds(g * cols, cols)],
            rows_in.at[g, pl.ds(own_row, own_tok), :],
            local_sems.at[g],
        ))
    own_cols = pl.ds(pl.multiple_of(core * ff_half, 128), ff_half)
    other_cols = pl.ds(pl.multiple_of(other * ff_half, 128), ff_half)
    own_ff = pl.ds(pl.multiple_of(core * ff_half, 128), ff_half)
    other_ff = pl.ds(pl.multiple_of(other * ff_half, 128), ff_half)
    loads.append(pltpu.make_async_copy(meta.at[core], metas.at[num_ep - 1], local_sems.at[col_groups]))
    for load in loads:
        load.start()
    weight_loads = [
        pltpu.make_async_copy(w_gate.at[0], wg.at[:, own_cols], local_sems.at[col_groups + 1]),
        pltpu.make_async_copy(w_up.at[0], wu.at[:, own_cols], local_sems.at[col_groups + 2]),
        pltpu.make_async_copy(w_down.at[0], wd.at[own_ff, :], local_sems.at[col_groups + 3]),
        pltpu.make_async_copy(gain, gains.at[core], local_sems.at[col_groups + 4]),
        pltpu.make_async_copy(bias, biases.at[core], local_sems.at[col_groups + 5]),
    ]

    barrier = pltpu.get_barrier_semaphore()
    for peer in (targets[0], targets[1], partner):
        pl.semaphore_signal(barrier, inc=1, device_id=peer, device_id_type=pl.DeviceIdType.MESH)
    pl.semaphore_wait(barrier, 3)

    for load in loads:
        load.wait()

    def row_half(direction, c):
        first = c // col_groups
        return first if direction == 0 else 1 - first

    def dispatch_copy(direction, step, c):
        r = row_half(direction, c)
        g = lax.rem(c, col_groups)
        src = jnp.where(step == 0, own_row, (step - 1) * slot_rows + direction * own_tok) + r * part
        dst = step * slot_rows + jnp.where(step == half - 1, 0, direction * own_tok) + r * part
        return pltpu.make_async_remote_copy(
            src_ref=rows_in.at[g, pl.ds(pl.multiple_of(src, part), part), :],
            dst_ref=rows_in.at[g, pl.ds(pl.multiple_of(dst, part), part), :],
            send_sem=disp_send.at[direction, lax.rem(step, 2), c],
            recv_sem=disp_recv.at[direction, step, c],
            device_id=targets[direction],
            device_id_type=pl.DeviceIdType.MESH,
        )

    def meta_copy(direction, step):
        src = jnp.where(step == 0, num_ep - 1, (step - 1) * 2 + direction)
        dst = step * 2 + direction
        return pltpu.make_async_remote_copy(
            src_ref=metas.at[src],
            dst_ref=metas.at[dst],
            send_sem=meta_send.at[direction, lax.rem(step, 2)],
            recv_sem=meta_recv.at[direction, step],
            device_id=targets[direction],
            device_id_type=pl.DeviceIdType.MESH,
        )

    for direction in range(2):
        meta_copy(direction, jnp.int32(0)).start()

    @pl.loop(0, chunks)
    def _(c):
        for direction in range(2):
            dispatch_copy(direction, jnp.int32(0), c).start()

    for load in weight_loads:
        load.start()

    def pair_copy(src, dst, k):
        return pltpu.make_async_remote_copy(
            src_ref=src, dst_ref=dst, send_sem=pair_sems.at[0, k], recv_sem=pair_sems.at[1, k],
            device_id=partner, device_id_type=pl.DeviceIdType.MESH,
        )

    gate_steps = first_pair * chunks
    gate_rows = width // gate_steps
    down_rows = 32
    down_steps = ff_half // down_rows
    pair_copy(gain, gains.at[core], 3).start()
    pair_copy(bias, biases.at[core], 4).start()

    def weight_step(kk):
        @pl.when(kk < gate_steps)
        def _():
            rows = pl.ds(pl.multiple_of(kk * gate_rows, gate_rows), gate_rows)
            pair_copy(w_gate.at[0, rows, :], wg.at[rows, own_cols], 0).start()
            pair_copy(w_up.at[0, rows, :], wu.at[rows, own_cols], 1).start()

        @pl.when((kk >= gate_steps) & (kk < gate_steps + down_steps))
        def _():
            at = (kk - gate_steps) * down_rows
            src = pl.ds(pl.multiple_of(at, down_rows), down_rows)
            dst = pl.ds(pl.multiple_of(core * ff_half + at, down_rows), down_rows)
            pair_copy(w_down.at[0, src, :], wd.at[dst, :], 2).start()

    def wait_weights():
        for load in weight_loads:
            load.wait()
        pair_copy(w_gate.at[0], wg.at[:, other_cols], 0).wait_recv()
        pair_copy(w_up.at[0], wu.at[:, other_cols], 1).wait_recv()
        pair_copy(w_down.at[0], wd.at[other_ff, :], 2).wait_recv()
        pair_copy(gain, gains.at[other], 3).wait_recv()
        pair_copy(bias, biases.at[other], 4).wait_recv()

    def weight_column(b):
        per_batch = ffn_rows // own_tok
        lane = lax.broadcasted_iota(jnp.int32, (own_tok, 128), 1)
        sub = lax.broadcasted_iota(jnp.int32, (own_tok, 128), 0)
        mine = lane * own_tok // 128 == sub
        for i in range(per_batch):
            block = metas[b * per_batch + i]
            flat = jnp.where(block[1:2, :] == me.astype(f32), block[0:1, :], 0.0)
            spread = jnp.where(mine, jnp.broadcast_to(flat, (own_tok, 128)), 0.0)
            column = jnp.sum(spread, axis=1, keepdims=True)
            weight_cols[pl.ds(i * own_tok, own_tok), :] = jnp.broadcast_to(column, (own_tok, 128))

    def gate_up(b, j):
        rows = pl.ds(pl.multiple_of(b * ffn_rows, ffn_rows), ffn_rows)
        at = pl.ds(pl.multiple_of(j * ffn_cols, ffn_cols), ffn_cols)
        gate = jnp.zeros((ffn_rows, ffn_cols), f32)
        upper = jnp.zeros((ffn_rows, ffn_cols), f32)
        for g in range(col_groups):
            x = rows_in[g, rows, :]
            gate += jnp.dot(x, wg[pl.ds(g * cols, cols), at], preferred_element_type=f32)
            upper += jnp.dot(x, wu[pl.ds(g * cols, cols), at], preferred_element_type=f32)
        value = gate / (1.0 + jnp.exp(-gate)) * upper * weight_cols[:, 0:1]
        hidden[j] = value.astype(bf16)

    def down(b, g):
        rows = pl.ds(pl.multiple_of(b * ffn_rows, ffn_rows), ffn_rows)
        at = pl.ds(pl.multiple_of(g * cols, cols), cols)
        total = jnp.zeros((ffn_rows, cols), f32)
        for j in range(ff_tiles):
            total += jnp.dot(hidden[j], wd[pl.ds(j * ffn_cols, ffn_cols), at], preferred_element_type=f32)
        sums[g, rows, :] = total

    def ffn_step(b, k):
        @pl.when(k == 0)
        def _():
            weight_column(b)

        @pl.when((lax.rem(k, 2) == 0) & (k < 2 * ff_tiles))
        def _():
            gate_up(b, k // 2)

        @pl.when((k >= 2 * ff_tiles) & (k < 2 * ff_tiles + col_groups))
        def _():
            down(b, k - 2 * ff_tiles)

    @pl.loop(0, half * chunks)
    def _(kk):
        slot = kk // chunks
        c = lax.rem(kk, chunks)
        step = slot + 1

        @pl.when(c == 0)
        def _():
            meta_copy(0, slot).wait_recv()

            @pl.when(step < half)
            def _():
                meta_copy(1, slot).wait_recv()

                @pl.when(step >= 2)
                def _():
                    meta_copy(0, step).wait_send()

                meta_copy(0, step).start()

                @pl.when(step < half - 1)
                def _():
                    @pl.when(step >= 2)
                    def _():
                        meta_copy(1, step).wait_send()

                    meta_copy(1, step).start()

        for direction in range(2):
            @pl.when((step < half) | (c < col_groups))
            def _():
                dispatch_copy(direction, slot, c).wait_recv()

            @pl.when((step < half - 1) | ((step == half - 1) & (c < col_groups)))
            def _():
                @pl.when(step >= 2)
                def _():
                    dispatch_copy(direction, step, c).wait_send()

                dispatch_copy(direction, step, c).start()

        weight_step(kk)
        pair = slot // 2

        @pl.when(kk == first_pair * 2 * chunks)
        def _():
            wait_weights()

        @pl.when(pair >= first_pair)
        def _():
            ffn_step(jnp.where(pair == pairs - 1, last - 1, pair - first_pair), lax.rem(kk, 2 * chunks))

    def chain_rows(age, r):
        return pl.ds(pl.multiple_of(age * own_tok + r * part, part), part)

    def sum_rows(distance, direction, r):
        at = (distance - 1) * slot_rows + jnp.where(distance == half, 0, (1 - direction) * own_tok) + r * part
        return pl.ds(pl.multiple_of(at, part), part)

    def combine_copy(direction, distance, c):
        r = row_half(direction, c)
        g = lax.rem(c, col_groups)
        return pltpu.make_async_remote_copy(
            src_ref=chain.at[direction, g, chain_rows(distance, r), :],
            dst_ref=chain.at[direction, g, chain_rows(distance - 1, r), :],
            send_sem=comb_send.at[direction, lax.rem(distance, 2), c],
            recv_sem=comb_recv.at[direction, distance - 1, c],
            device_id=targets[direction],
            device_id_type=pl.DeviceIdType.MESH,
        )

    weight_column(last)

    @pl.loop(0, ff_tiles)
    def _(j):
        gate_up(last, j)

    @pl.loop(0, col_groups)
    def _(g):
        down(last, g)
        for direction in range(2):
            r = direction
            chain[direction, g, chain_rows(half, r), :] = sums[g, sum_rows(half, direction, r), :].astype(bf16)
            combine_copy(direction, jnp.int32(half), g).start()

    @pl.loop(chunks, half * chunks)
    def _(kk):
        distance = half - kk // chunks
        c = lax.rem(kk, chunks)
        g = lax.rem(c, col_groups)
        for direction in range(2):
            r = row_half(direction, c)
            fresh = (distance == half - 1) & (c >= col_groups)
            mine = sums[g, sum_rows(distance, direction, r), :]

            @pl.when(fresh)
            def _():
                chain[direction, g, chain_rows(distance, r), :] = mine.astype(bf16)

            @pl.when(jnp.logical_not(fresh))
            def _():
                combine_copy(direction, distance + 1, c).wait_recv()
                before = chain[direction, g, chain_rows(distance, r), :].astype(f32)
                chain[direction, g, chain_rows(distance, r), :] = (before + mine).astype(bf16)

            @pl.when((distance <= half - 3) | ((distance == half - 2) & (c < col_groups)))
            def _():
                combine_copy(direction, distance, c).wait_send()

            combine_copy(direction, distance, c).start()

        batch = last - 2 - (kk - chunks) // (2 * chunks)

        @pl.when(batch >= ahead)
        def _():
            ffn_step(batch, lax.rem(kk - chunks, 2 * chunks))

    row_sum = jnp.zeros((own_tok, 1), f32)
    for direction in range(2):
        @pl.loop(0, chunks)
        def _(c):
            combine_copy(direction, jnp.int32(1), c).wait_recv()
    kept = []
    for g in range(col_groups):
        mixture = (
            chain[0, g, 0:own_tok, :].astype(f32)
            + chain[1, g, 0:own_tok, :].astype(f32)
            + sums[g, pl.ds(own_row, own_tok), :]
        ).astype(bf16)
        value = residual_scale * rows_in[g, pl.ds(own_row, own_tok), :].astype(f32) + mixture.astype(f32)
        sums[g, pl.ds(own_row, own_tok), :] = value
        row_sum += jnp.sum(value, axis=1, keepdims=True)
    mean = row_sum / width
    square_sum = jnp.zeros((own_tok, 1), f32)
    for g in range(col_groups):
        value = sums[g, pl.ds(own_row, own_tok), :] - mean
        square_sum += jnp.sum(value * value, axis=1, keepdims=True)
    scale = lax.rsqrt(square_sum / width + norm_eps)
    per_half = col_groups // 2
    for g in range(col_groups):
        at = pl.ds((g % per_half) * cols, cols)
        value = (sums[g, pl.ds(own_row, own_tok), :] - mean) * scale
        own_out[g] = (value * gains[g // per_half, :, at] + biases[g // per_half, :, at]).astype(bf16)
    swap = pair_copy(own_out.at[pl.ds(other * per_half, per_half)], other_out, 5)
    swap.start()
    for g in range(per_half):
        out[pl.ds(core * own_tok, own_tok), pl.ds(g * cols, cols)] = own_out[core * per_half + g]
    swap.wait_recv()
    for g in range(per_half):
        out[pl.ds(other * own_tok, own_tok), pl.ds(g * cols, cols)] = other_out[g]

    swap.wait_send()
    for direction in range(2):
        @pl.loop(0, chunks)
        def _(c):
            for step in (half - 2, half - 1):
                dispatch_copy(direction, jnp.int32(step), c).wait_send()
            for distance in (2, 1):
                combine_copy(direction, jnp.int32(distance), c).wait_send()
        for step in (half - 2, half - 1):
            meta_copy(direction, jnp.int32(step)).wait_send()
    pair_copy(w_gate.at[0], wg.at[:, own_cols], 0).wait_send()
    pair_copy(w_up.at[0], wu.at[:, own_cols], 1).wait_send()
    pair_copy(w_down.at[0], wd.at[own_ff, :], 2).wait_send()
    pair_copy(gain, gains.at[core], 3).wait_send()
    pair_copy(bias, biases.at[core], 4).wait_send()


def shards(tokens, routes, gate_weights, w_gate, w_up, w_down, norm_gain, norm_bias):
    num_ep = lax.axis_size("ep")
    tok_rows, width = tokens.shape
    own_tok = tok_rows // 2
    half = num_ep // 2
    ff = 2 * w_down.shape[1]
    cols = width // col_groups
    chunks = 2 * col_groups
    rows = half * 2 * own_tok
    meta = jnp.stack(
        [gate_weights.reshape(2, own_tok * gate_weights.shape[1]), routes.astype(f32).reshape(2, own_tok * routes.shape[1])],
        axis=1,
    )
    any_spec = pl.BlockSpec(memory_space=pl.ANY)
    dma = pltpu.SemaphoreType.DMA
    return pl.pallas_call(
        functools.partial(moe_kernel, num_ep, num_ep),
        out_shape=jax.ShapeDtypeStruct((tok_rows, width // 2), bf16),
        in_specs=[any_spec] * 7,
        out_specs=pl.BlockSpec(memory_space=pltpu.VMEM),
        scratch_shapes=[
            pltpu.VMEM((col_groups, rows, cols), bf16),
            pltpu.VMEM((num_ep, 2, 128), f32),
            pltpu.VMEM((width, ff), bf16),
            pltpu.VMEM((width, ff), bf16),
            pltpu.VMEM((ff, width), bf16),
            pltpu.VMEM((2, 1, width // 2), f32),
            pltpu.VMEM((2, 1, width // 2), f32),
            pltpu.VMEM((ffn_rows, 128), f32),
            pltpu.VMEM((ff // ffn_cols, ffn_rows, ffn_cols), bf16),
            pltpu.VMEM((col_groups, rows, cols), f32),
            pltpu.VMEM((2, col_groups, (half + 1) * own_tok, cols), bf16),
            pltpu.VMEM((col_groups, own_tok, cols), bf16),
            pltpu.VMEM((col_groups // 2, own_tok, cols), bf16),
            dma((2, half, chunks)),
            dma((2, 2, chunks)),
            dma((2, half)),
            dma((2, 2)),
            dma((2, half, chunks)),
            dma((2, 2, chunks)),
            dma((col_groups + 6,)),
            dma((2, 6)),
        ],
        compiler_params=pltpu.CompilerParams(
            collective_id=0, has_side_effects=True, vmem_limit_bytes=60 * 1024 * 1024
        ),
    )(tokens, meta, w_gate, w_up, w_down, norm_gain.reshape(1, -1), norm_bias.reshape(1, -1))


def solution(mesh):
    in_specs = (
        P(("grp", "ep"), None),
        P(("grp", "ep"), None),
        P(("grp", "ep"), None),
        P("ep", None, "tp"),
        P("ep", None, "tp"),
        P("ep", "tp", None),
        P("tp"),
        P("tp"),
    )
    out_specs = P(("grp", "ep"), "tp")
    return jax.shard_map(shards, mesh=mesh, in_specs=in_specs, out_specs=out_specs, check_vma=False)
```

```python
import functools

import jax
import jax.numpy as jnp
from jax import lax
from jax.experimental import pallas as pl
from jax.experimental.pallas import tpu as pltpu
from jax.sharding import PartitionSpec as P

residual_scale = 1.4142135
norm_eps = 1e-05
col_groups = 4
ffn_cols = 256
down_steps = 2
bf16, f32 = jnp.bfloat16, jnp.float32


def hops_of(num_ep):
    longer = 2 * ((9 * num_ep) // 32)
    return longer, num_ep - 1 - longer


def moe_kernel(
    num_ep,
    tokens, meta, w_gate, w_up, w_down, gain, bias, out,
    rows_in, metas, wg, wu, wd, gains, biases, weight_cols, hidden, sums, chain, swap_in, own_out, other_out,
    disp_recv, disp_send, meta_recv, meta_send, comb_recv, comb_send, swap_sems, local_sems, pair_sems,
):
    me = lax.axis_index("ep")
    core = lax.axis_index("tp")
    other = 1 - core
    longer, shorter = hops_of(num_ep)
    hops = jnp.where(core == 1, longer, shorter)
    tok, width = tokens.shape
    half_tok = tok // 2
    cols = width // col_groups
    ff_half = w_down.shape[1]
    ff = 2 * ff_half
    ff_tiles = ff // ffn_cols
    chunks = col_groups
    shift = jnp.where(core == 1, 1, 0)
    own_slot = jnp.where(core == 1, longer, 0)
    batches = (hops + 1) // 2
    first_pair = batches // 2
    last = batches - 1
    up, under = lax.rem(me + 1, num_ep), lax.rem(me + num_ep - 1, num_ep)
    disp_target = {"ep": jnp.where(core == 1, up, under)}
    comb_target = {"ep": jnp.where(core == 1, under, up)}
    partner = {"tp": other}
    mesh_ids = pl.DeviceIdType.MESH

    def slot_rows(slot):
        return pl.ds(pl.multiple_of(slot * tok, tok), tok)

    loads = [
        pltpu.make_async_copy(tokens.at[:, pl.ds(g * cols, cols)], rows_in.at[g, slot_rows(own_slot), :], local_sems.at[g])
        for g in range(col_groups)
    ]
    loads.append(pltpu.make_async_copy(meta, metas.at[own_slot], local_sems.at[col_groups]))
    for load in loads:
        load.start()
    own_cols = pl.ds(pl.multiple_of(core * ff_half, 128), ff_half)
    other_cols = pl.ds(pl.multiple_of(other * ff_half, 128), ff_half)
    weight_loads = [
        pltpu.make_async_copy(w_gate.at[0], wg.at[:, own_cols], local_sems.at[col_groups + 1]),
        pltpu.make_async_copy(w_up.at[0], wu.at[:, own_cols], local_sems.at[col_groups + 2]),
        pltpu.make_async_copy(w_down.at[0], wd.at[own_cols, :], local_sems.at[col_groups + 3]),
        pltpu.make_async_copy(gain, gains.at[core], local_sems.at[col_groups + 4]),
        pltpu.make_async_copy(bias, biases.at[core], local_sems.at[col_groups + 5]),
    ]

    barrier = pltpu.get_barrier_semaphore()
    for peer in ({"ep": up}, {"ep": under}, partner):
        pl.semaphore_signal(barrier, inc=1, device_id=peer, device_id_type=mesh_ids)
    pl.semaphore_wait(barrier, 3)

    for load in loads:
        load.wait()

    def slot_of(age):
        return jnp.where(age == 0, own_slot, age - shift)

    def dispatch_copy(age, c):
        return pltpu.make_async_remote_copy(
            src_ref=rows_in.at[c, slot_rows(slot_of(age)), :],
            dst_ref=rows_in.at[c, slot_rows(age + 1 - shift), :],
            send_sem=disp_send.at[lax.rem(age, 2), c],
            recv_sem=disp_recv.at[age, c],
            device_id=disp_target,
            device_id_type=mesh_ids,
        )

    def meta_copy(age):
        return pltpu.make_async_remote_copy(
            src_ref=metas.at[slot_of(age)],
            dst_ref=metas.at[age + 1 - shift],
            send_sem=meta_send.at[lax.rem(age, 2)],
            recv_sem=meta_recv.at[age],
            device_id=disp_target,
            device_id_type=mesh_ids,
        )

    def combine_copy(distance, c):
        return pltpu.make_async_remote_copy(
            src_ref=chain.at[c, slot_rows(distance), :],
            dst_ref=chain.at[c, slot_rows(distance - 1), :],
            send_sem=comb_send.at[lax.rem(distance, 2), c],
            recv_sem=comb_recv.at[distance - 1, c],
            device_id=comb_target,
            device_id_type=mesh_ids,
        )

    def pair_copy(src, dst, k):
        return pltpu.make_async_remote_copy(
            src_ref=src, dst_ref=dst, send_sem=pair_sems.at[0, k], recv_sem=pair_sems.at[1, k],
            device_id=partner, device_id_type=mesh_ids,
        )

    meta_copy(jnp.int32(0)).start()
    for c in range(chunks):
        dispatch_copy(jnp.int32(0), c).start()
    for load in weight_loads:
        load.start()
    pair_copy(gain, gains.at[core], 3).start()
    pair_copy(bias, biases.at[core], 4).start()

    free_steps = chunks * (2 * (((shorter + 1) // 2) // 2) - 1)
    gate_steps = 1 << (free_steps.bit_length() - 1)
    gate_rows = width // gate_steps
    down_rows = ff_half // free_steps

    def weight_step(kk):
        @pl.when(kk < gate_steps)
        def _():
            rows = pl.ds(pl.multiple_of(kk * gate_rows, gate_rows), gate_rows)
            pair_copy(w_gate.at[0, rows, :], wg.at[rows, own_cols], 0).start()
            pair_copy(w_up.at[0, rows, :], wu.at[rows, own_cols], 1).start()

        @pl.when(kk < free_steps)
        def _():
            src = pl.ds(pl.multiple_of(kk * down_rows, down_rows), down_rows)
            dst = pl.ds(pl.multiple_of(core * ff_half + kk * down_rows, down_rows), down_rows)
            pair_copy(w_down.at[0, src, :], wd.at[dst, :], 2).start()

    def wait_weights():
        for load in weight_loads:
            load.wait()
        pair_copy(w_gate.at[0], wg.at[:, other_cols], 0).wait_recv()
        pair_copy(w_up.at[0], wu.at[:, other_cols], 1).wait_recv()
        pair_copy(w_down.at[0], wd.at[other_cols, :], 2).wait_recv()
        pair_copy(gain, gains.at[other], 3).wait_recv()
        pair_copy(bias, biases.at[other], 4).wait_recv()

    def weight_column(b):
        pairs_per_block = meta.shape[1]
        lane = lax.broadcasted_iota(jnp.int32, (tok, pairs_per_block), 1)
        sub = lax.broadcasted_iota(jnp.int32, (tok, pairs_per_block), 0)
        mine = lane * tok // pairs_per_block == sub
        for i in range(2):
            block = metas[b * 2 + i]
            flat = jnp.where(block[1:2, :] == me.astype(f32), block[0:1, :], 0.0)
            spread = jnp.where(mine, jnp.broadcast_to(flat, (tok, pairs_per_block)), 0.0)
            column = jnp.sum(spread, axis=1, keepdims=True)
            weight_cols[pl.ds(i * tok, tok), :] = jnp.broadcast_to(column, (tok, 128))

    def batch_rows(b):
        return pl.ds(pl.multiple_of(b * 2 * tok, 2 * tok), 2 * tok)

    def gate_up(b, j):
        at = pl.ds(pl.multiple_of(j * ffn_cols, ffn_cols), ffn_cols)
        gate = jnp.zeros((2 * tok, ffn_cols), f32)
        upper = jnp.zeros((2 * tok, ffn_cols), f32)
        for g in range(col_groups):
            x = rows_in[g, batch_rows(b), :]
            gate += jnp.dot(x, wg[pl.ds(g * cols, cols), at], preferred_element_type=f32)
            upper += jnp.dot(x, wu[pl.ds(g * cols, cols), at], preferred_element_type=f32)
        value = gate / (1.0 + jnp.exp(-gate)) * upper * weight_cols[:, 0:1]
        hidden[j] = value.astype(bf16)

    def down(b, g):
        at = pl.ds(pl.multiple_of(g * cols, cols), cols)
        total = jnp.zeros((2 * tok, cols), f32)
        for j in range(ff_tiles):
            total += jnp.dot(hidden[j], wd[pl.ds(j * ffn_cols, ffn_cols), at], preferred_element_type=f32)
        sums[g, batch_rows(b), :] = total

    def ffn_step(b, k):
        @pl.when(k == 0)
        def _():
            weight_column(b)

        @pl.when(k < ff_tiles)
        def _():
            gate_up(b, k)

        @pl.when((k >= ff_tiles) & (k < ff_tiles + down_steps))
        def _():
            for i in range(col_groups // down_steps):
                down(b, (k - ff_tiles) * (col_groups // down_steps) + i)

    @pl.loop(0, hops * chunks)
    def _(kk):
        age = kk // chunks
        c = lax.rem(kk, chunks)
        forward = age + 1 < hops

        @pl.when(c == 0)
        def _():
            meta_copy(age).wait_recv()

            @pl.when(forward)
            def _():
                @pl.when(age >= 1)
                def _():
                    meta_copy(age + 1).wait_send()

                meta_copy(age + 1).start()

        dispatch_copy(age, c).wait_recv()

        @pl.when(forward)
        def _():
            @pl.when(age >= 1)
            def _():
                dispatch_copy(age + 1, c).wait_send()

            dispatch_copy(age + 1, c).start()

        weight_step(kk)
        slot = age + 1 - shift
        pair = slot // 2
        k = lax.rem(slot, 2) * chunks + c

        @pl.when((pair == first_pair) & (k == 0))
        def _():
            wait_weights()

        @pl.when(pair >= first_pair)
        def _():
            ffn_step(jnp.where(pair == last, last - 1, pair - first_pair), k)

    weight_column(last)

    @pl.loop(0, ff_tiles)
    def _(j):
        gate_up(last, j)

    @pl.loop(0, chunks)
    def _(g):
        down(last, g)
        chain[g, slot_rows(hops), :] = sums[g, slot_rows(hops - shift), :].astype(bf16)
        combine_copy(hops, g).start()

    @pl.loop(0, (hops - 1) * chunks)
    def _(kk):
        distance = hops - 1 - kk // chunks
        c = lax.rem(kk, chunks)
        combine_copy(distance + 1, c).wait_recv()
        before = chain[c, slot_rows(distance), :].astype(f32)
        chain[c, slot_rows(distance), :] = (before + sums[c, slot_rows(distance - shift), :]).astype(bf16)

        @pl.when(distance <= hops - 2)
        def _():
            combine_copy(distance, c).wait_send()

        combine_copy(distance, c).start()
        pair = kk // (2 * chunks)
        batch = last - 2 - pair

        @pl.when(batch >= last - first_pair)
        def _():
            ffn_step(batch, lax.rem(kk, 2 * chunks))

    own_half = pl.ds(pl.multiple_of(core * half_tok, half_tok), half_tok)
    other_half = pl.ds(pl.multiple_of(other * half_tok, half_tok), half_tok)

    def swap_copy(g):
        return pltpu.make_async_remote_copy(
            src_ref=chain.at[g, other_half, :], dst_ref=swap_in.at[g],
            send_sem=swap_sems.at[0, g], recv_sem=swap_sems.at[1, g],
            device_id=partner, device_id_type=mesh_ids,
        )

    for g in range(col_groups):
        combine_copy(jnp.int32(1), g).wait_recv()

        @pl.when(core == 0)
        def _():
            chain[g, 0:tok, :] = (chain[g, 0:tok, :].astype(f32) + sums[g, 0:tok, :]).astype(bf16)

        swap_copy(g).start()
    own_rows = pl.ds(pl.multiple_of(own_slot * tok + core * half_tok, half_tok), half_tok)
    row_sum = jnp.zeros((half_tok, 1), f32)
    for g in range(col_groups):
        swap_copy(g).wait_recv()
        mixture = (chain[g, own_half, :].astype(f32) + swap_in[g].astype(f32)).astype(bf16)
        value = residual_scale * rows_in[g, own_rows, :].astype(f32) + mixture.astype(f32)
        sums[g, own_half, :] = value
        row_sum += jnp.sum(value, axis=1, keepdims=True)
    mean = row_sum / width
    square_sum = jnp.zeros((half_tok, 1), f32)
    for g in range(col_groups):
        value = sums[g, own_half, :] - mean
        square_sum += jnp.sum(value * value, axis=1, keepdims=True)
    scale = lax.rsqrt(square_sum / width + norm_eps)
    per_half = col_groups // 2
    for g in range(col_groups):
        at = pl.ds((g % per_half) * cols, cols)
        value = (sums[g, own_half, :] - mean) * scale
        own_out[g] = (value * gains[g // per_half, :, at] + biases[g // per_half, :, at]).astype(bf16)
    trade = pair_copy(own_out.at[pl.ds(other * per_half, per_half)], other_out, 5)
    trade.start()
    for g in range(per_half):
        out[own_half, pl.ds(g * cols, cols)] = own_out[core * per_half + g]
    trade.wait_recv()
    for g in range(per_half):
        out[other_half, pl.ds(g * cols, cols)] = other_out[g]

    trade.wait_send()
    for c in range(chunks):
        swap_copy(c).wait_send()
        for back in (2, 1):
            dispatch_copy(hops - back, c).wait_send()
            combine_copy(jnp.int32(back), c).wait_send()
    for back in (2, 1):
        meta_copy(hops - back).wait_send()
    pair_copy(w_gate.at[0], wg.at[:, own_cols], 0).wait_send()
    pair_copy(w_up.at[0], wu.at[:, own_cols], 1).wait_send()
    pair_copy(w_down.at[0], wd.at[own_cols, :], 2).wait_send()
    pair_copy(gain, gains.at[core], 3).wait_send()
    pair_copy(bias, biases.at[core], 4).wait_send()


def shards(tokens, routes, gate_weights, w_gate, w_up, w_down, norm_gain, norm_bias):
    num_ep = lax.axis_size("ep")
    tok, width = tokens.shape
    ff = 2 * w_down.shape[1]
    cols = width // col_groups
    slots = hops_of(num_ep)[0] + 1
    pairs_per_block = routes.size
    meta = jnp.stack([gate_weights.reshape(pairs_per_block), routes.astype(f32).reshape(pairs_per_block)])
    any_spec = pl.BlockSpec(memory_space=pl.ANY)
    dma = pltpu.SemaphoreType.DMA
    return pl.pallas_call(
        functools.partial(moe_kernel, num_ep),
        out_shape=jax.ShapeDtypeStruct((tok, width // 2), bf16),
        in_specs=[any_spec] * 7,
        out_specs=pl.BlockSpec(memory_space=pltpu.VMEM),
        scratch_shapes=[
            pltpu.VMEM((col_groups, slots * tok, cols), bf16),
            pltpu.VMEM((slots, 2, pairs_per_block), f32),
            pltpu.VMEM((width, ff), bf16),
            pltpu.VMEM((width, ff), bf16),
            pltpu.VMEM((ff, width), bf16),
            pltpu.VMEM((2, 1, width // 2), f32),
            pltpu.VMEM((2, 1, width // 2), f32),
            pltpu.VMEM((2 * tok, 128), f32),
            pltpu.VMEM((ff // ffn_cols, 2 * tok, ffn_cols), bf16),
            pltpu.VMEM((col_groups, slots * tok, cols), f32),
            pltpu.VMEM((col_groups, slots * tok, cols), bf16),
            pltpu.VMEM((col_groups, tok // 2, cols), bf16),
            pltpu.VMEM((col_groups, tok // 2, cols), bf16),
            pltpu.VMEM((col_groups // 2, tok // 2, cols), bf16),
            dma((slots, col_groups)),
            dma((2, col_groups)),
            dma((slots,)),
            dma((2,)),
            dma((slots, col_groups)),
            dma((2, col_groups)),
            dma((2, col_groups)),
            dma((col_groups + 6,)),
            dma((2, 6)),
        ],
        compiler_params=pltpu.CompilerParams(
            collective_id=0, has_side_effects=True, vmem_limit_bytes=60 * 1024 * 1024
        ),
    )(tokens, meta, w_gate, w_up, w_down, norm_gain.reshape(1, -1), norm_bias.reshape(1, -1))


def solution(mesh):
    in_specs = (
        P(("grp", "ep"), None),
        P(("grp", "ep"), None),
        P(("grp", "ep"), None),
        P("ep", None, "tp"),
        P("ep", None, "tp"),
        P("ep", "tp", None),
        P("tp"),
        P("tp"),
    )
    out_specs = P(("grp", "ep"), "tp")
    return jax.shard_map(shards, mesh=mesh, in_specs=in_specs, out_specs=out_specs, check_vma=False)
```

```python
import functools

import jax
import jax.numpy as jnp
from jax import lax
from jax.experimental import pallas as pl
from jax.experimental.pallas import tpu as pltpu
from jax.sharding import PartitionSpec as P

residual_scale = 1.4142135
norm_eps = 1e-05
col_groups = 4
ffn_cols = 256
down_steps = 2
bf16, f32 = jnp.bfloat16, jnp.float32


def hops_of(num_ep):
    longer = (17 * num_ep // 32) | 1
    return longer, num_ep - 1 - longer


def moe_kernel(
    num_ep,
    tokens, routes, gate_weights, w_gate, w_up, w_down, out,
    rows_in, routes_in, gates_in, metas, wg, wu, wd, weight_cols, hidden, sums, chain, swap_in, own_out,
    disp_recv, disp_send, meta_recv, meta_send, comb_recv, comb_send, swap_sems, local_sems, pair_sems,
):
    me = lax.axis_index("ep")
    core = lax.axis_index("tp")
    other = 1 - core
    longer, shorter = hops_of(num_ep)
    hops = jnp.where(core == 1, longer, shorter)
    tok, width = tokens.shape
    half_tok = tok // 2
    top = routes.shape[0]
    cols = width // col_groups
    ff_half = w_down.shape[1]
    ff = 2 * ff_half
    ff_tiles = ff // ffn_cols
    chunks = col_groups
    shift = jnp.where(core == 1, 0, 1)
    own_slot = jnp.where(core == 1, 0, shorter)
    batches = (hops + 1) // 2
    first_pair = batches // 2
    last = batches - 1
    up, under = lax.rem(me + 1, num_ep), lax.rem(me + num_ep - 1, num_ep)
    disp_target = {"ep": jnp.where(core == 1, up, under)}
    comb_target = {"ep": jnp.where(core == 1, under, up)}
    partner = {"tp": other}
    mesh_ids = pl.DeviceIdType.MESH

    def slot_rows(slot):
        return pl.ds(pl.multiple_of(slot * tok, tok), tok)

    loads = [
        pltpu.make_async_copy(tokens.at[:, pl.ds(g * cols, cols)], rows_in.at[g, slot_rows(own_slot), :], local_sems.at[g])
        for g in range(col_groups)
    ]
    loads.append(pltpu.make_async_copy(routes, routes_in, local_sems.at[col_groups]))
    loads.append(pltpu.make_async_copy(gate_weights, gates_in, local_sems.at[col_groups + 4]))
    for load in loads:
        load.start()
    own_cols = pl.ds(pl.multiple_of(core * ff_half, 128), ff_half)
    other_cols = pl.ds(pl.multiple_of(other * ff_half, 128), ff_half)
    weight_loads = [
        pltpu.make_async_copy(w_gate.at[0], wg.at[:, own_cols], local_sems.at[col_groups + 1]),
        pltpu.make_async_copy(w_up.at[0], wu.at[:, own_cols], local_sems.at[col_groups + 2]),
        pltpu.make_async_copy(w_down.at[0], wd.at[own_cols, :], local_sems.at[col_groups + 3]),
    ]

    barrier = pltpu.get_barrier_semaphore()
    for peer in ({"ep": up}, {"ep": under}, partner):
        pl.semaphore_signal(barrier, inc=1, device_id=peer, device_id_type=mesh_ids)

    for load in loads:
        load.wait()
    lane = lax.broadcasted_iota(jnp.int32, (tok, tok), 1)
    sub = lax.broadcasted_iota(jnp.int32, (tok, tok), 0)
    metas[own_slot, 0:top, :] = routes_in[...].astype(f32)
    metas[own_slot, top:2 * top, :] = gates_in[...]
    pl.semaphore_wait(barrier, 3)

    def slot_of(age):
        return jnp.where(age == 0, own_slot, age - shift)

    def dispatch_copy(age, c):
        return pltpu.make_async_remote_copy(
            src_ref=rows_in.at[c, slot_rows(slot_of(age)), :],
            dst_ref=rows_in.at[c, slot_rows(age + 1 - shift), :],
            send_sem=disp_send.at[lax.rem(age, 2), c],
            recv_sem=disp_recv.at[age, c],
            device_id=disp_target,
            device_id_type=mesh_ids,
        )

    def meta_copy(age):
        return pltpu.make_async_remote_copy(
            src_ref=metas.at[slot_of(age)],
            dst_ref=metas.at[age + 1 - shift],
            send_sem=meta_send.at[lax.rem(age, 2)],
            recv_sem=meta_recv.at[age],
            device_id=disp_target,
            device_id_type=mesh_ids,
        )

    def combine_copy(distance, c):
        return pltpu.make_async_remote_copy(
            src_ref=chain.at[c, slot_rows(distance), :],
            dst_ref=chain.at[c, slot_rows(distance - 1), :],
            send_sem=comb_send.at[lax.rem(distance, 2), c],
            recv_sem=comb_recv.at[distance - 1, c],
            device_id=comb_target,
            device_id_type=mesh_ids,
        )

    def pair_copy(src, dst, k):
        return pltpu.make_async_remote_copy(
            src_ref=src, dst_ref=dst, send_sem=pair_sems.at[0, k], recv_sem=pair_sems.at[1, k],
            device_id=partner, device_id_type=mesh_ids,
        )

    for c in range(chunks):
        dispatch_copy(jnp.int32(0), c).start()
    meta_copy(jnp.int32(0)).start()
    for load in weight_loads:
        load.start()

    free_steps = min(chunks * 2 * (shorter // 4), ff_half // 32)
    gate_steps = 1 << (free_steps.bit_length() - 1)
    gate_rows = width // gate_steps
    down_rows = ff_half // free_steps

    def weight_step(kk):
        @pl.when(kk < gate_steps)
        def _():
            rows = pl.ds(pl.multiple_of(kk * gate_rows, gate_rows), gate_rows)
            pair_copy(w_gate.at[0, rows, :], wg.at[rows, own_cols], 0).start()
            pair_copy(w_up.at[0, rows, :], wu.at[rows, own_cols], 1).start()

        @pl.when(kk < free_steps)
        def _():
            src = pl.ds(pl.multiple_of(kk * down_rows, down_rows), down_rows)
            dst = pl.ds(pl.multiple_of(core * ff_half + kk * down_rows, down_rows), down_rows)
            pair_copy(w_down.at[0, src, :], wd.at[dst, :], 2).start()

    def wait_weights():
        for load in weight_loads:
            load.wait()
        pair_copy(w_gate.at[0], wg.at[:, other_cols], 0).wait_recv()
        pair_copy(w_up.at[0], wu.at[:, other_cols], 1).wait_recv()
        pair_copy(w_down.at[0], wd.at[other_cols, :], 2).wait_recv()

    def weight_column(b):
        for i in range(2):
            block = metas[b * 2 + i]
            row = jnp.zeros((1, tok), f32)
            for k in range(top):
                row += jnp.where(block[k:k + 1, :] == me.astype(f32), block[top + k:top + k + 1, :], 0.0)
            spread = jnp.where(lane == sub, jnp.broadcast_to(row, (tok, tok)), 0.0)
            column = jnp.sum(spread, axis=1, keepdims=True)
            weight_cols[pl.ds(i * tok, tok), :] = jnp.broadcast_to(column, (tok, 128))

    def batch_rows(b):
        return pl.ds(pl.multiple_of(b * 2 * tok, 2 * tok), 2 * tok)

    def gate_up(b, j):
        at = pl.ds(pl.multiple_of(j * ffn_cols, ffn_cols), ffn_cols)
        gate = jnp.zeros((2 * tok, ffn_cols), f32)
        upper = jnp.zeros((2 * tok, ffn_cols), f32)
        for g in range(col_groups):
            x = rows_in[g, batch_rows(b), :]
            gate += jnp.dot(x, wg[pl.ds(g * cols, cols), at], preferred_element_type=f32)
            upper += jnp.dot(x, wu[pl.ds(g * cols, cols), at], preferred_element_type=f32)
        value = gate / (1.0 + jnp.exp(-gate)) * upper * weight_cols[:, 0:1]
        hidden[j] = value.astype(bf16)

    def down(b, g):
        at = pl.ds(pl.multiple_of(g * cols, cols), cols)
        total = jnp.zeros((2 * tok, cols), f32)
        for j in range(ff_tiles):
            total += jnp.dot(hidden[j], wd[pl.ds(j * ffn_cols, ffn_cols), at], preferred_element_type=f32)
        sums[g, batch_rows(b), :] = total

    def ffn_step(b, k):
        @pl.when(k == 0)
        def _():
            weight_column(b)

        @pl.when(k < ff_tiles)
        def _():
            gate_up(b, k)

        @pl.when((k >= ff_tiles) & (k < ff_tiles + down_steps))
        def _():
            for i in range(col_groups // down_steps):
                down(b, (k - ff_tiles) * (col_groups // down_steps) + i)

    @pl.loop(0, hops * chunks)
    def _(kk):
        age = kk // chunks
        c = lax.rem(kk, chunks)
        forward = age + 1 < hops

        @pl.when(forward & (age >= 1))
        def _():
            dispatch_copy(age + 1, c).wait_send()

        dispatch_copy(age, c).wait_recv()

        @pl.when(forward)
        def _():
            dispatch_copy(age + 1, c).start()

        @pl.when(c == chunks - 1)
        def _():
            meta_copy(age).wait_recv()

            @pl.when(forward)
            def _():
                @pl.when(age >= 1)
                def _():
                    meta_copy(age + 1).wait_send()

                meta_copy(age + 1).start()

        weight_step(kk)
        slot = age + 1 - shift
        pair = slot // 2
        k = lax.rem(slot, 2) * chunks + c

        @pl.when((pair == first_pair) & (k == 0))
        def _():
            wait_weights()

        @pl.when(pair >= first_pair)
        def _():
            ffn_step(jnp.where(pair == last, last - 1, pair - first_pair), k)

    weight_column(last)

    @pl.loop(0, ff_tiles)
    def _(j):
        gate_up(last, j)

    @pl.loop(0, chunks)
    def _(g):
        down(last, g)
        chain[g, slot_rows(hops), :] = sums[g, slot_rows(hops - shift), :].astype(bf16)
        combine_copy(hops, g).start()

    @pl.loop(0, (hops - 1) * chunks)
    def _(kk):
        distance = hops - 1 - kk // chunks
        c = lax.rem(kk, chunks)
        @pl.when(distance <= hops - 2)
        def _():
            combine_copy(distance, c).wait_send()

        combine_copy(distance + 1, c).wait_recv()
        before = chain[c, slot_rows(distance), :].astype(f32)
        chain[c, slot_rows(distance), :] = (before + sums[c, slot_rows(distance - shift), :]).astype(bf16)

        combine_copy(distance, c).start()
        pair = kk // (2 * chunks)
        batch = last - 2 - pair

        @pl.when(batch >= last - first_pair)
        def _():
            ffn_step(batch, lax.rem(kk, 2 * chunks))

    own_half = pl.ds(pl.multiple_of(core * half_tok, half_tok), half_tok)
    other_half = pl.ds(pl.multiple_of(other * half_tok, half_tok), half_tok)

    def swap_copy(g):
        return pltpu.make_async_remote_copy(
            src_ref=chain.at[g, other_half, :], dst_ref=swap_in.at[g],
            send_sem=swap_sems.at[0, g], recv_sem=swap_sems.at[1, g],
            device_id=partner, device_id_type=mesh_ids,
        )

    for g in range(col_groups):
        combine_copy(jnp.int32(1), g).wait_recv()

        @pl.when(core == 1)
        def _():
            chain[g, 0:tok, :] = (chain[g, 0:tok, :].astype(f32) + sums[g, 0:tok, :]).astype(bf16)

        swap_copy(g).start()
    own_rows = pl.ds(pl.multiple_of(own_slot * tok + core * half_tok, half_tok), half_tok)
    row_sum = jnp.zeros((half_tok, 1), f32)
    for g in range(col_groups):
        swap_copy(g).wait_recv()
        mixture = (chain[g, own_half, :].astype(f32) + swap_in[g].astype(f32)).astype(bf16)
        value = residual_scale * rows_in[g, own_rows, :].astype(f32) + mixture.astype(f32)
        sums[g, own_half, :] = value
        row_sum += jnp.sum(value, axis=1, keepdims=True)
    mean = row_sum / width
    square_sum = jnp.zeros((half_tok, 1), f32)
    for g in range(col_groups):
        value = sums[g, own_half, :] - mean
        square_sum += jnp.sum(value * value, axis=1, keepdims=True)
    scale = lax.rsqrt(square_sum / width + norm_eps)
    per_half = col_groups // 2
    for g in range(col_groups):
        own_out[g] = (sums[g, own_half, :] - mean) * scale
    trades = [
        pltpu.make_async_remote_copy(
            src_ref=own_out.at[other * per_half + g], dst_ref=out.at[own_half, pl.ds(g * cols, cols)],
            send_sem=pair_sems.at[0, 3 + g], recv_sem=pair_sems.at[1, 3 + g],
            device_id=partner, device_id_type=mesh_ids,
        )
        for g in range(per_half)
    ]
    for trade in trades:
        trade.start()
    for g in range(per_half):
        out[own_half, pl.ds(g * cols, cols)] = own_out[core * per_half + g]
    for trade in trades:
        trade.wait_recv()

    for trade in trades:
        trade.wait_send()
    for c in range(chunks):
        swap_copy(c).wait_send()
        for back in (2, 1):
            dispatch_copy(hops - back, c).wait_send()
            combine_copy(jnp.int32(back), c).wait_send()
    for back in (2, 1):
        meta_copy(hops - back).wait_send()
    pair_copy(w_gate.at[0], wg.at[:, own_cols], 0).wait_send()
    pair_copy(w_up.at[0], wu.at[:, own_cols], 1).wait_send()
    pair_copy(w_down.at[0], wd.at[own_cols, :], 2).wait_send()


def shards(tokens, routes, gate_weights, w_gate, w_up, w_down, norm_gain, norm_bias):
    num_ep = lax.axis_size("ep")
    tok, width = tokens.shape
    ff = 2 * w_down.shape[1]
    cols = width // col_groups
    slots = hops_of(num_ep)[0] + 1
    any_spec = pl.BlockSpec(memory_space=pl.ANY)
    dma = pltpu.SemaphoreType.DMA
    rows = pl.pallas_call(
        functools.partial(moe_kernel, num_ep),
        out_shape=jax.ShapeDtypeStruct((tok, width // 2), f32),
        in_specs=[any_spec] * 6,
        out_specs=pl.BlockSpec(memory_space=pltpu.VMEM),
        scratch_shapes=[
            pltpu.VMEM((col_groups, slots * tok, cols), bf16),
            pltpu.VMEM(routes.shape[::-1], jnp.int32),
            pltpu.VMEM(routes.shape[::-1], f32),
            pltpu.VMEM((slots, 2 * routes.shape[1], tok), f32),
            pltpu.VMEM((width, ff), bf16),
            pltpu.VMEM((width, ff), bf16),
            pltpu.VMEM((ff, width), bf16),
            pltpu.VMEM((2 * tok, 128), f32),
            pltpu.VMEM((ff // ffn_cols, 2 * tok, ffn_cols), bf16),
            pltpu.VMEM((col_groups, slots * tok, cols), f32),
            pltpu.VMEM((col_groups, slots * tok, cols), bf16),
            pltpu.VMEM((col_groups, tok // 2, cols), bf16),
            pltpu.VMEM((col_groups, tok // 2, cols), f32),
            dma((slots, col_groups)),
            dma((2, col_groups)),
            dma((slots,)),
            dma((2,)),
            dma((slots, col_groups)),
            dma((2, col_groups)),
            dma((2, col_groups)),
            dma((col_groups + 6,)),
            dma((2, 6)),
        ],
        compiler_params=pltpu.CompilerParams(
            collective_id=0, has_side_effects=True, vmem_limit_bytes=60 * 1024 * 1024
        ),
    )(tokens, routes.T, gate_weights.T, w_gate, w_up, w_down)
    return (rows * norm_gain + norm_bias).astype(bf16)


def solution(mesh):
    in_specs = (
        P(("grp", "ep"), None),
        P(("grp", "ep"), None),
        P(("grp", "ep"), None),
        P("ep", None, "tp"),
        P("ep", None, "tp"),
        P("ep", "tp", None),
        P("tp"),
        P("tp"),
    )
    out_specs = P(("grp", "ep"), "tp")
    return jax.shard_map(shards, mesh=mesh, in_specs=in_specs, out_specs=out_specs, check_vma=False)
```

```python
import functools

import jax
import jax.numpy as jnp
from jax import lax
from jax.experimental import pallas as pl
from jax.experimental.pallas import tpu as pltpu
from jax.sharding import PartitionSpec as P

residual_scale = 1.4142135
norm_eps = 1e-05
col_groups = 4
ffn_cols = 256
down_steps = 2
bf16, f32 = jnp.bfloat16, jnp.float32


def hops_of(num_ep):
    longer = (17 * num_ep // 32) | 1
    return longer, num_ep - 1 - longer


def moe_kernel(
    num_ep,
    tokens, routes, gate_weights, w_gate, w_up, w_down, out,
    rows_in, routes_in, gates_in, metas, wg, wu, wd, weight_cols, hidden, sums, chain, swap_in, own_out,
    disp_recv, disp_send, meta_recv, meta_send, comb_recv, comb_send, swap_sems, local_sems, pair_sems,
):
    me = lax.axis_index("ep")
    core = lax.axis_index("tp")
    other = 1 - core
    longer, shorter = hops_of(num_ep)
    hops = jnp.where(core == 1, longer, shorter)
    tok, width = tokens.shape
    half_tok = tok // 2
    top = routes.shape[0]
    cols = width // col_groups
    ff_half = w_down.shape[1]
    ff = 2 * ff_half
    ff_tiles = ff // ffn_cols
    chunks = col_groups
    shift = jnp.where(core == 1, 0, 1)
    own_slot = jnp.where(core == 1, 0, shorter)
    batches = (hops + 1) // 2
    first_pair = batches // 2
    last = batches - 1
    up, under = lax.rem(me + 1, num_ep), lax.rem(me + num_ep - 1, num_ep)
    disp_target = {"ep": jnp.where(core == 1, up, under)}
    comb_target = {"ep": jnp.where(core == 1, under, up)}
    partner = {"tp": other}
    mesh_ids = pl.DeviceIdType.MESH

    def slot_rows(slot):
        return pl.ds(pl.multiple_of(slot * tok, tok), tok)

    loads = [
        pltpu.make_async_copy(tokens.at[:, pl.ds(g * cols, cols)], rows_in.at[g, slot_rows(own_slot), :], local_sems.at[g])
        for g in range(col_groups)
    ]
    loads.append(pltpu.make_async_copy(routes, routes_in, local_sems.at[col_groups]))
    loads.append(pltpu.make_async_copy(gate_weights, gates_in, local_sems.at[col_groups + 4]))
    for load in loads:
        load.start()
    own_cols = pl.ds(pl.multiple_of(core * ff_half, 128), ff_half)
    other_cols = pl.ds(pl.multiple_of(other * ff_half, 128), ff_half)
    weight_loads = [
        pltpu.make_async_copy(w_gate.at[0], wg.at[:, own_cols], local_sems.at[col_groups + 1]),
        pltpu.make_async_copy(w_up.at[0], wu.at[:, own_cols], local_sems.at[col_groups + 2]),
        pltpu.make_async_copy(w_down.at[0], wd.at[own_cols, :], local_sems.at[col_groups + 3]),
    ]

    barrier = pltpu.get_barrier_semaphore()
    for peer in ({"ep": up}, {"ep": under}, partner):
        pl.semaphore_signal(barrier, inc=1, device_id=peer, device_id_type=mesh_ids)

    for load in loads:
        load.wait()
    lane = lax.broadcasted_iota(jnp.int32, (tok, tok), 1)
    sub = lax.broadcasted_iota(jnp.int32, (tok, tok), 0)
    metas[own_slot, 0:top, :] = routes_in[...].astype(f32)
    metas[own_slot, top:2 * top, :] = gates_in[...]
    pl.semaphore_wait(barrier, 3)

    def slot_of(age):
        return jnp.where(age == 0, own_slot, age - shift)

    def dispatch_copy(age, c):
        return pltpu.make_async_remote_copy(
            src_ref=rows_in.at[c, slot_rows(slot_of(age)), :],
            dst_ref=rows_in.at[c, slot_rows(age + 1 - shift), :],
            send_sem=disp_send.at[lax.rem(age, 2), c],
            recv_sem=disp_recv.at[age, c],
            device_id=disp_target,
            device_id_type=mesh_ids,
        )

    def meta_copy(age):
        return pltpu.make_async_remote_copy(
            src_ref=metas.at[slot_of(age)],
            dst_ref=metas.at[age + 1 - shift],
            send_sem=meta_send.at[lax.rem(age, 2)],
            recv_sem=meta_recv.at[age],
            device_id=disp_target,
            device_id_type=mesh_ids,
        )

    def combine_copy(distance, c):
        return pltpu.make_async_remote_copy(
            src_ref=chain.at[c, slot_rows(distance), :],
            dst_ref=chain.at[c, slot_rows(distance - 1), :],
            send_sem=comb_send.at[lax.rem(distance, 2), c],
            recv_sem=comb_recv.at[distance - 1, c],
            device_id=comb_target,
            device_id_type=mesh_ids,
        )

    def pair_copy(src, dst, k):
        return pltpu.make_async_remote_copy(
            src_ref=src, dst_ref=dst, send_sem=pair_sems.at[0, k], recv_sem=pair_sems.at[1, k],
            device_id=partner, device_id_type=mesh_ids,
        )

    for c in range(chunks):
        dispatch_copy(jnp.int32(0), c).start()
    meta_copy(jnp.int32(0)).start()
    for load in weight_loads:
        load.start()

    free_steps = min(chunks * 2 * (shorter // 4), ff_half // 32)
    gate_steps = 1 << (free_steps.bit_length() - 1)
    gate_rows = width // gate_steps
    down_rows = ff_half // free_steps

    def weight_step(kk):
        @pl.when(kk < gate_steps)
        def _():
            rows = pl.ds(pl.multiple_of(kk * gate_rows, gate_rows), gate_rows)
            pair_copy(w_gate.at[0, rows, :], wg.at[rows, own_cols], 0).start()
            pair_copy(w_up.at[0, rows, :], wu.at[rows, own_cols], 1).start()

        @pl.when(kk < free_steps)
        def _():
            src = pl.ds(pl.multiple_of(kk * down_rows, down_rows), down_rows)
            dst = pl.ds(pl.multiple_of(core * ff_half + kk * down_rows, down_rows), down_rows)
            pair_copy(w_down.at[0, src, :], wd.at[dst, :], 2).start()

    def wait_weights():
        for load in weight_loads:
            load.wait()
        pair_copy(w_gate.at[0], wg.at[:, other_cols], 0).wait_recv()
        pair_copy(w_up.at[0], wu.at[:, other_cols], 1).wait_recv()
        pair_copy(w_down.at[0], wd.at[other_cols, :], 2).wait_recv()

    def weight_column(b):
        for i in range(2):
            block = metas[b * 2 + i]
            row = jnp.zeros((1, tok), f32)
            for k in range(top):
                row += jnp.where(block[k:k + 1, :] == me.astype(f32), block[top + k:top + k + 1, :], 0.0)
            spread = jnp.where(lane == sub, jnp.broadcast_to(row, (tok, tok)), 0.0)
            column = jnp.sum(spread, axis=1, keepdims=True)
            weight_cols[pl.ds(i * tok, tok), :] = jnp.broadcast_to(column, (tok, 128))

    def batch_rows(b):
        return pl.ds(pl.multiple_of(b * 2 * tok, 2 * tok), 2 * tok)

    def gate_up(b, j):
        at = pl.ds(pl.multiple_of(j * ffn_cols, ffn_cols), ffn_cols)
        gate = jnp.zeros((2 * tok, ffn_cols), f32)
        upper = jnp.zeros((2 * tok, ffn_cols), f32)
        for g in range(col_groups):
            x = rows_in[g, batch_rows(b), :]
            gate += jnp.dot(x, wg[pl.ds(g * cols, cols), at], preferred_element_type=f32)
            upper += jnp.dot(x, wu[pl.ds(g * cols, cols), at], preferred_element_type=f32)
        value = gate / (1.0 + jnp.exp(-gate)) * upper * weight_cols[:, 0:1]
        hidden[j] = value.astype(bf16)

    def down(b, g):
        at = pl.ds(pl.multiple_of(g * cols, cols), cols)
        total = jnp.zeros((2 * tok, cols), f32)
        for j in range(ff_tiles):
            total += jnp.dot(hidden[j], wd[pl.ds(j * ffn_cols, ffn_cols), at], preferred_element_type=f32)
        sums[g, batch_rows(b), :] = total

    def ffn_step(b, k):
        @pl.when(k == 0)
        def _():
            weight_column(b)

        @pl.when(k < ff_tiles)
        def _():
            gate_up(b, k)

        @pl.when((k >= ff_tiles) & (k < ff_tiles + down_steps))
        def _():
            for i in range(col_groups // down_steps):
                down(b, (k - ff_tiles) * (col_groups // down_steps) + i)

    @pl.loop(0, hops * chunks)
    def _(kk):
        age = kk // chunks
        c = lax.rem(kk, chunks)
        forward = age + 1 < hops

        @pl.when(forward & (age >= 1))
        def _():
            dispatch_copy(age + 1, c).wait_send()

        dispatch_copy(age, c).wait_recv()

        @pl.when(forward)
        def _():
            dispatch_copy(age + 1, c).start()

        @pl.when(c == chunks - 1)
        def _():
            meta_copy(age).wait_recv()

            @pl.when(forward)
            def _():
                @pl.when(age >= 1)
                def _():
                    meta_copy(age + 1).wait_send()

                meta_copy(age + 1).start()

        weight_step(kk)
        slot = age + 1 - shift
        pair = slot // 2
        k = lax.rem(slot, 2) * chunks + c

        @pl.when((pair == first_pair) & (k == 0))
        def _():
            wait_weights()

        @pl.when(pair >= first_pair)
        def _():
            ffn_step(jnp.where(pair == last, last - 1, pair - first_pair), k)

    weight_column(last)

    for j in range(ff_tiles):
        gate_up(last, j)
    for g in range(chunks):
        down(last, g)
        chain[g, slot_rows(hops), :] = sums[g, slot_rows(hops - shift), :].astype(bf16)
        combine_copy(hops, g).start()

    @pl.loop(0, (hops - 1) * chunks)
    def _(kk):
        distance = hops - 1 - kk // chunks
        c = lax.rem(kk, chunks)
        @pl.when(distance <= hops - 2)
        def _():
            combine_copy(distance, c).wait_send()

        combine_copy(distance + 1, c).wait_recv()
        before = chain[c, slot_rows(distance), :].astype(f32)
        chain[c, slot_rows(distance), :] = (before + sums[c, slot_rows(distance - shift), :]).astype(bf16)

        combine_copy(distance, c).start()
        pair = kk // (2 * chunks)
        batch = last - 2 - pair

        @pl.when(batch >= last - first_pair)
        def _():
            ffn_step(batch, lax.rem(kk, 2 * chunks))

    own_half = pl.ds(pl.multiple_of(core * half_tok, half_tok), half_tok)
    other_half = pl.ds(pl.multiple_of(other * half_tok, half_tok), half_tok)

    def swap_copy(g):
        return pltpu.make_async_remote_copy(
            src_ref=chain.at[g, other_half, :], dst_ref=swap_in.at[g],
            send_sem=swap_sems.at[0, g], recv_sem=swap_sems.at[1, g],
            device_id=partner, device_id_type=mesh_ids,
        )

    for g in range(col_groups):
        combine_copy(jnp.int32(1), g).wait_recv()

        @pl.when(core == 1)
        def _():
            chain[g, 0:tok, :] = (chain[g, 0:tok, :].astype(f32) + sums[g, 0:tok, :]).astype(bf16)

        swap_copy(g).start()
    own_rows = pl.ds(pl.multiple_of(own_slot * tok + core * half_tok, half_tok), half_tok)
    row_sum = jnp.zeros((half_tok, 1), f32)
    for g in range(col_groups):
        swap_copy(g).wait_recv()
        mixture = (chain[g, own_half, :].astype(f32) + swap_in[g].astype(f32)).astype(bf16)
        value = residual_scale * rows_in[g, own_rows, :].astype(f32) + mixture.astype(f32)
        sums[g, own_half, :] = value
        row_sum += jnp.sum(value, axis=1, keepdims=True)
    mean = row_sum / width
    square_sum = jnp.zeros((half_tok, 1), f32)
    for g in range(col_groups):
        value = sums[g, own_half, :] - mean
        square_sum += jnp.sum(value * value, axis=1, keepdims=True)
    scale = lax.rsqrt(square_sum / width + norm_eps)
    per_half = col_groups // 2
    for g in range(col_groups):
        own_out[g] = (sums[g, own_half, :] - mean) * scale
    trades = [
        pltpu.make_async_remote_copy(
            src_ref=own_out.at[other * per_half + g], dst_ref=out.at[own_half, pl.ds(g * cols, cols)],
            send_sem=pair_sems.at[0, 3 + g], recv_sem=pair_sems.at[1, 3 + g],
            device_id=partner, device_id_type=mesh_ids,
        )
        for g in range(per_half)
    ]
    for trade in trades:
        trade.start()
    for g in range(per_half):
        out[own_half, pl.ds(g * cols, cols)] = own_out[core * per_half + g]
    for trade in trades:
        trade.wait_recv()

    for trade in trades:
        trade.wait_send()
    for c in range(chunks):
        swap_copy(c).wait_send()
        for back in (2, 1):
            dispatch_copy(hops - back, c).wait_send()
            combine_copy(jnp.int32(back), c).wait_send()
    for back in (2, 1):
        meta_copy(hops - back).wait_send()
    pair_copy(w_gate.at[0], wg.at[:, own_cols], 0).wait_send()
    pair_copy(w_up.at[0], wu.at[:, own_cols], 1).wait_send()
    pair_copy(w_down.at[0], wd.at[own_cols, :], 2).wait_send()


def shards(tokens, routes, gate_weights, w_gate, w_up, w_down, norm_gain, norm_bias):
    num_ep = lax.axis_size("ep")
    tok, width = tokens.shape
    ff = 2 * w_down.shape[1]
    cols = width // col_groups
    slots = hops_of(num_ep)[0] + 1
    any_spec = pl.BlockSpec(memory_space=pl.ANY)
    dma = pltpu.SemaphoreType.DMA
    rows = pl.pallas_call(
        functools.partial(moe_kernel, num_ep),
        out_shape=jax.ShapeDtypeStruct((tok, width // 2), f32),
        in_specs=[any_spec] * 6,
        out_specs=pl.BlockSpec(memory_space=pltpu.VMEM),
        scratch_shapes=[
            pltpu.VMEM((col_groups, slots * tok, cols), bf16),
            pltpu.VMEM(routes.shape[::-1], jnp.int32),
            pltpu.VMEM(routes.shape[::-1], f32),
            pltpu.VMEM((slots, 2 * routes.shape[1], tok), f32),
            pltpu.VMEM((width, ff), bf16),
            pltpu.VMEM((width, ff), bf16),
            pltpu.VMEM((ff, width), bf16),
            pltpu.VMEM((2 * tok, 128), f32),
            pltpu.VMEM((ff // ffn_cols, 2 * tok, ffn_cols), bf16),
            pltpu.VMEM((col_groups, slots * tok, cols), f32),
            pltpu.VMEM((col_groups, slots * tok, cols), bf16),
            pltpu.VMEM((col_groups, tok // 2, cols), bf16),
            pltpu.VMEM((col_groups, tok // 2, cols), f32),
            dma((slots, col_groups)),
            dma((2, col_groups)),
            dma((slots,)),
            dma((2,)),
            dma((slots, col_groups)),
            dma((2, col_groups)),
            dma((2, col_groups)),
            dma((col_groups + 6,)),
            dma((2, 6)),
        ],
        compiler_params=pltpu.CompilerParams(
            collective_id=0, has_side_effects=True, vmem_limit_bytes=60 * 1024 * 1024
        ),
    )(tokens, routes.T, gate_weights.T, w_gate, w_up, w_down)
    return (rows * norm_gain + norm_bias).astype(bf16)


def solution(mesh):
    in_specs = (
        P(("grp", "ep"), None),
        P(("grp", "ep"), None),
        P(("grp", "ep"), None),
        P("ep", None, "tp"),
        P("ep", None, "tp"),
        P("ep", "tp", None),
        P("tp"),
        P("tp"),
    )
    out_specs = P(("grp", "ep"), "tp")
    return jax.shard_map(shards, mesh=mesh, in_specs=in_specs, out_specs=out_specs, check_vma=False)
```
